128 devices in a mesh: kv: 16 (over z, y), tp: 8 (over x, core).
Axes of the slice: x: 4, y: 4, z: 4, core: 2. Of those that a mesh axis runs over, the one named last changes fastest.
Arguments:
- tokens: bfloat16 [16, 4096], P(None, 'kv'), may hold values from -6 to 6
- norm_gain: float32 [4096], P('kv'), may hold values from 0.1 to 1.9
- query_weight: bfloat16 [4096, 2048], P('kv', 'tp'), may hold values from -1 to 1
- key_weight: bfloat16 [4096, 2048], P('kv', 'tp'), may hold values from -0.09375 to 0.09375
- value_weight: bfloat16 [4096, 2048], P('kv', 'tp'), may hold values from -0.09375 to 0.09375
- out_weight: bfloat16 [2048, 4096], P('tp', 'kv'), may hold values from -0.125 to 0.125
- lambdas: float32 [16], P('tp'), may hold values from 0.3 to 0.8
- head_gain: float32 [128], replicated, may hold values from 0.1 to 1.9
- lengths: int32 [16], replicated, may hold values from 1 to 16383, as said below
- key_cache: bfloat16 [16, 16384, 16, 128], P(None, 'kv', 'tp'), may hold values from -48 to 48, as said below
- value_cache: bfloat16 [16, 16384, 16, 128], P(None, 'kv', 'tp'), may hold values from -6 to 6
Outputs:
- attended: bfloat16 [16, 4096], P(None, 'kv')
The draws below stay inside these ranges and needn't reach their ends.
Inputs may be any that keep to these rules, and one draw needn't show every extreme that they name: `lengths`: each sequence has 1 to 16383 cached tokens. `key_cache`: cached keys lie between -48 and 48.
All inputs are finite; a program needn't handle non-finite values.
Results may differ from the reference program's by a relative error of at most 0.012.
The reference program's roundings to bfloat16 on the way (of `normed`, `fresh_value`, `weights` and `head_out`) count: a program that leaves them out, or rounds other values in their place, can miss the bound.
Values may be sent and summed in bfloat16 or wider, within the bound.
A program may use at most 64 MiB of HBM per device.

```python
import jax
import jax.numpy as jnp
from jax import lax

D = 4096
H = 16
DH = 64
SEQS = 16
POS_DEV = 1024
CACHE_LEN = 16384
N_KV = 16


def token_values(key):
    base = jax.random.fold_in(key, 11)
    drawn = jnp.clip(jax.random.normal(base, (SEQS, D), jnp.float32), -6.0, 6.0)
    return drawn.astype(jnp.bfloat16)


def gain_values(key):
    base = jax.random.fold_in(key, 12)
    drawn = 1.0 + 0.18 * jnp.clip(jax.random.normal(base, (D,), jnp.float32), -5.0, 5.0)
    return drawn


def weight_values(key):
    base = jax.random.fold_in(key, 13)
    whole_shape = (D, H * 2 * DH)
    drawn = jnp.clip(jax.random.normal(base, whole_shape, jnp.float32), -6.0, 6.0)
    return (drawn * D ** (-0.5)).astype(jnp.bfloat16)


def length_values(key):
    base = jax.random.fold_in(key, 14)
    return jax.random.randint(base, (SEQS,), 1, CACHE_LEN).astype(jnp.int32)


def draw_tokens(key, part):
    return token_values(key)


def draw_norm_gain(key, part):
    return gain_values(key)


def draw_query_weight(key, part):
    return weight_values(key)


def draw_lengths(key, part):
    return length_values(key)


def draw_key_cache(key, part):
    base = jax.random.fold_in(key, 15)
    whole_shape = (SEQS, CACHE_LEN, H, 2 * DH)
    drawn = jnp.clip(1.5 * jax.random.normal(base, whole_shape, jnp.float32), -9.0, 9.0)
    return drawn.astype(jnp.bfloat16)


def levels(rng, shape, cuts, low, largest):
    factor_of, own = 1.0, jax.random.fold_in(rng, 6)
    for dim, shards_of in cuts:
        heights = jnp.exp(jax.random.uniform(jax.random.fold_in(own, dim), (shards_of,), jnp.float32, low / len(cuts), largest / len(cuts)))
        factor_of = factor_of * jnp.repeat(heights, shape[dim] // shards_of).reshape([-1 if axis == dim else 1 for axis in range(len(shape))])
    return factor_of


def centred(stream_key, shape, deviation, reach, pieces=(), kind=jnp.bfloat16):
    gain = levels(stream_key, shape, pieces, -0.22, 0.18) if pieces else 1.0
    entries = jax.random.normal(stream_key, shape, jnp.float32) * deviation * gain
    return jnp.minimum(jnp.maximum(entries, -reach), reach).astype(kind)


def setup_inputs(seed: int = 0) -> dict:
    splits = jax.random.split(jax.random.key(seed), 12)
    tokens = draw_tokens(jax.random.fold_in(splits[11], 71), 0)
    norm_gain = draw_norm_gain(jax.random.fold_in(splits[11], 71), 0)
    query_weight = draw_query_weight(jax.random.fold_in(splits[11], 71), 0)
    key_weight = centred(splits[3], (D, H * 2 * DH), D ** -0.5, 0.09375, ((0, 16), (1, 8)))
    value_weight = centred(splits[4], (D, H * 2 * DH), D ** -0.5, 0.09375, ((0, 16), (1, 8)))
    out_weight = centred(splits[5], (H * 2 * DH, D), (H * 2 * DH) ** -0.5, 0.125, ((0, 8), (1, 16)))
    lambdas = jnp.clip(0.3 + 0.5 * jax.random.uniform(splits[6], (H,), jnp.float32) ** levels(splits[6], (H,), ((0, 8),), -0.2, 0.2), 0.3, 0.8)
    head_gain = jnp.clip(1.0 + 0.18 * jax.random.normal(splits[7], (2 * DH,), jnp.float32), 0.1, 1.9)
    lengths = draw_lengths(jax.random.fold_in(splits[11], 71), 0)
    key_cache = draw_key_cache(jax.random.fold_in(splits[11], 71), 0)
    value_cache = centred(splits[10], (SEQS, CACHE_LEN, H, 2 * DH), 1.0, 6.0, ((1, 16), (2, 8)))
    return {"tokens": tokens, "norm_gain": norm_gain, "query_weight": query_weight, "key_weight": key_weight, "value_weight": value_weight, "out_weight": out_weight, "lambdas": lambdas, "head_gain": head_gain, "lengths": lengths, "key_cache": key_cache, "value_cache": value_cache}


epsilon = 1e-05
theta_base = 500000.0
floor_value = -1e+30

def angles_for(positions, width):
    halfway = width // 2
    frequency = theta_base ** (-jnp.arange(halfway, dtype=jnp.float32) / halfway)
    return positions.astype(jnp.float32)[:, None] * frequency[None, :]

def rotate(values_in, angles):
    halfway = values_in.shape[-1] // 2
    cosine = jnp.cos(angles)[:, None, None, :]
    sine_part = jnp.sin(angles)[:, None, None, :]
    former = values_in[..., :halfway]
    latter = values_in[..., halfway:]
    return jnp.concatenate([former * cosine - latter * sine_part, latter * cosine + former * sine_part], axis=-1)

def reference(tokens, norm_gain, query_weight, key_weight, value_weight, out_weight, lambdas, head_gain, lengths, key_cache, value_cache):
    widened = tokens.astype(jnp.float32)
    row_scale = lax.rsqrt(lax.optimization_barrier(jnp.sum(widened * widened, axis=1)) / D + epsilon)
    normed = (widened * norm_gain[None, :]).astype(jnp.bfloat16)

    def project(weight):
        return jnp.dot(normed, weight, preferred_element_type=jnp.float32) * row_scale[:, None]
    angles = angles_for(lengths, DH)
    query = rotate(project(query_weight).reshape(SEQS, H, 2, DH), angles).astype(jnp.bfloat16)
    fresh_key = rotate(project(key_weight).reshape(SEQS, H, 2, DH), angles).astype(jnp.bfloat16)
    fresh_value = project(value_weight).reshape(SEQS, H, 2 * DH).astype(jnp.bfloat16)

    def per_block(block_index):
        offset = block_index * POS_DEV
        positions = offset + jnp.arange(POS_DEV, dtype=jnp.int32)
        key_block = lax.dynamic_slice_in_dim(key_cache, offset, POS_DEV, 1).reshape(SEQS, POS_DEV, H, 2, DH)
        value_block = lax.dynamic_slice_in_dim(value_cache, offset, POS_DEV, 1)
        at_length = positions[None, :] == lengths[:, None]
        key_block = jnp.where(at_length[:, :, None, None, None], fresh_key[:, None], key_block)
        value_block = jnp.where(at_length[:, :, None, None], fresh_value[:, None], value_block)
        scores = jnp.einsum('shjd,sphjd->shjp', query.astype(jnp.float32), key_block.astype(jnp.float32)) * DH ** (-0.5)
        visible = (positions[None, :] <= lengths[:, None])[:, None, None, :]
        masked = jnp.where(visible, scores, floor_value)
        block_max = lax.optimization_barrier(jnp.max(masked, axis=-1))
        weights = jnp.where(visible, jnp.exp(masked - block_max[..., None]), 0.0).astype(jnp.bfloat16)
        block_total = lax.optimization_barrier(jnp.sum(weights.astype(jnp.float32), axis=-1))
        block_values = jnp.einsum('shjp,sphe->shje', weights.astype(jnp.float32), value_block.astype(jnp.float32))
        return (block_max, block_total, block_values)
    maxima, totals, valued = lax.map(per_block, jnp.arange(N_KV, dtype=jnp.int32))
    highest = lax.optimization_barrier(jnp.max(maxima, axis=0))
    factor = jnp.exp(maxima - highest[None])
    total = lax.optimization_barrier(jnp.sum(totals * factor, axis=0))
    weighted = lax.optimization_barrier(jnp.sum(valued * factor[..., None], axis=0))
    mixed_heads = weighted[:, :, 0] / total[:, :, 0, None] - lambdas[None, :, None] * weighted[:, :, 1] / total[:, :, 1, None]
    head_out = mixed_heads * lax.rsqrt(lax.optimization_barrier(jnp.mean(mixed_heads * mixed_heads, axis=-1, keepdims=True)) + epsilon) * head_gain
    head_out = head_out.astype(jnp.bfloat16).reshape(SEQS, H * 2 * DH)
    return jnp.dot(head_out, out_weight, preferred_element_type=jnp.float32).astype(jnp.bfloat16)
```

```python
import functools

import jax
import jax.numpy as jnp
import numpy as np
from jax import lax
from jax.experimental import pallas as pl
from jax.experimental.pallas import tpu as pltpu
from jax.sharding import PartitionSpec as P

D = 4096
DH = 64
SEQS = 16
N_KV = 16
N_TP = 8
SIDE = 4
POS = 1024
ROWS = 2 * POS
EPS = 1e-05
THETA = 500000.0
FLOOR = -1e30
MESH = pl.DeviceIdType.MESH

ORDER = ((0, 0), (0, 1), (1, 0), (3, 0), (1, 1), (3, 1), (2, 0), (2, 1))
PAIRS = len(ORDER)
GROUPS = ((0, 3), (3, 5), (5, 7), (7, 9))
TILES = PAIRS + 1
STEPS = sorted(
    ((a, b) for a in range(SIDE) for b in range(SIDE) if a or b),
    key=lambda ab: min(ab[0], SIDE - ab[0]) + min(ab[1], SIDE - ab[1]),
)


def frequencies():
    half = DH // 2
    one = np.float64(THETA) ** (-np.arange(half, dtype=np.float64) / half)
    return np.tile(one.astype(np.float32), 2 * 128 // DH)[None, :]


def pair_of(kv, step):
    z, y = kv // SIDE, kv % SIDE
    return ((z + step[0]) % SIDE) * 2 + (y // 2 + step[1]) % 2


TURN = [[[pair_of(kv, st) for st in ORDER].index(q) for q in range(PAIRS)] for kv in range(N_KV)]


def tile(i, n=1):
    start = i * 8
    return pl.ds(start if isinstance(i, int) else pl.multiple_of(start, 8), 8 * n)


def kernel(
    tokens, gain, wq, wk, wv, wo, lambdas, head_gain, lengths, freq, keys, vals,
    out,
    tok_v, gain_v, wq_v, wk_v, wv_v, wo_v, lam_s, hg_v, len_s, freq_v, kbuf, vbuf,
    tx1, rx1, txa, rxa, obuf, rx2, ho, part, rx3,
    in_sem, k_sem, v_sem, s1, r1, sa, ra, s2, r2, s3, r3,
):
    me = lax.axis_index("kv")
    tp = lax.axis_index("tp")
    z, y = me // SIDE, me % SIDE

    def kv_peer(step):
        return ((z + step[0]) % SIDE) * SIDE + (y + step[1]) % SIDE

    def kv_peers():
        return [kv_peer(st) for st in STEPS]

    def tp_peers():
        return [(tp + d) % N_TP for d in range(1, N_TP)]

    barrier = pltpu.get_barrier_semaphore()
    for p in kv_peers():
        pl.semaphore_signal(barrier, 1, device_id=(p, tp), device_id_type=MESH)
    for p in tp_peers():
        pl.semaphore_signal(barrier, 1, device_id=(me, p), device_id_type=MESH)

    ins = [
        pltpu.make_async_copy(src, dst, in_sem.at[i])
        for i, (src, dst) in enumerate(
            (
                (tokens, tok_v), (gain, gain_v), (wq, wq_v), (wk, wk_v), (wv, wv_v), (lengths, len_s),
                (freq, freq_v), (lambdas, lam_s), (head_gain, hg_v), (wo, wo_v),
            )
        )
    ]
    for c in ins:
        c.start()
    pair_at = [pair_of(me, st) for st in ORDER]
    kin, vin = [], []
    for i, q in enumerate(pair_at):
        rows = pl.ds(2 * q, 2)
        kin.append(pltpu.make_async_copy(keys.at[rows], kbuf.at[rows], k_sem.at[i]))
        vin.append(pltpu.make_async_copy(vals.at[rows], vbuf.at[rows], v_sem.at[i]))
    for a, b in zip(kin, vin):
        a.start()
        b.start()

    lane = lax.broadcasted_iota(jnp.int32, (8, 128), 1)
    row = lax.broadcasted_iota(jnp.int32, (8, 128), 0)

    for c in ins[:2]:
        c.wait()
    widened = tok_v[...].astype(jnp.float32)
    squares = jnp.sum(widened * widened, axis=1, keepdims=True)
    normed = (widened * gain_v[...]).astype(jnp.bfloat16)
    low = lax.broadcasted_iota(jnp.int32, (SEQS, 128), 1) < DH
    ins[2].wait()
    q_part = jnp.dot(normed, wq_v[...], preferred_element_type=jnp.float32)
    ins[3].wait()
    k_part = jnp.dot(normed, wk_v[...], preferred_element_type=jnp.float32)
    ins[4].wait()
    v_part = jnp.dot(normed, wv_v[...], preferred_element_type=jnp.float32)
    q0, q1 = q_part[:, :128], q_part[:, 128:]
    lines = (
        jnp.where(low, q0, squares), jnp.where(low, q1, 0.0), jnp.where(low, 0.0, q0), jnp.where(low, 0.0, q1),
        k_part[:, :128], k_part[:, 128:], v_part[:, :128], v_part[:, 128:],
    )
    for i, line in enumerate(lines):
        tx1[pl.ds(i, SEQS, stride=8), :] = line

    pl.semaphore_wait(barrier, N_KV - 1 + N_TP - 1)

    for p in kv_peers():
        pltpu.make_async_remote_copy(
            tx1.at[tile(p)], rx1.at[tile(me)], s1, r1, device_id=(p, tp), device_id_type=MESH
        ).start()
    rx1[tile(me), :] = tx1[tile(me), :]

    ins[5].wait()
    ins[6].wait()
    own_length = len_s[me]
    angles = own_length.astype(jnp.float32) * freq_v[...]
    first = (lane & 32) == 0
    turned = row < 6
    cosine = jnp.where(turned, jnp.broadcast_to(jnp.cos(angles), (8, 128)), 1.0)
    sine = jnp.broadcast_to(jnp.sin(angles), (8, 128))
    sine = jnp.where(turned, jnp.where(first, -sine, sine), 0.0)

    whole = tx1.at[tile(0, N_KV - 1)]
    pltpu.make_async_copy(whole, whole, r1).wait()
    sums = [rx1[tile(i), :] for i in range(N_KV)]
    while len(sums) > 1:
        sums = [a + b for a, b in zip(sums[::2], sums[1::2])]
    summed = sums[0]
    scaling = lax.rsqrt(summed[0:1, DH : DH + 1] / D + EPS)
    x = jnp.where((row == 0) & (lane >= DH), 0.0, summed) * scaling
    other = jnp.where(first, pltpu.roll(x, 96, 1), pltpu.roll(x, 32, 1))
    x = (x * cosine + other * sine).astype(jnp.bfloat16).astype(jnp.float32)
    x = jnp.where(row < 4, x * DH ** (-0.5), x)
    x = jnp.where(lax.broadcast(me % 2, (8, 128)) == 1, pltpu.roll(x, 4, 0), x)
    txa[...] = x
    for p in kv_peers():
        pltpu.make_async_remote_copy(
            txa, rxa.at[tile(me)], sa, ra.at[me], device_id=(p, tp), device_id_type=MESH
        ).start()
    rxa[tile(me), :] = x

    column = lax.broadcasted_iota(jnp.int32, (8, 256), 1)
    crow = lax.broadcasted_iota(jnp.int32, (8, 256), 0)
    apart = ((column ^ crow) & 1) == 1
    offset = me * POS
    upper = row < 4

    ml = jnp.zeros((8, 128), jnp.float32)
    for i, q in enumerate(pair_at):
        a, b = 2 * q, 2 * q + 1
        if i == 0:
            other_one = me + 1 - 2 * (me % 2)
            pltpu.make_async_copy(txa, txa, ra.at[other_one]).wait()
        else:
            pltpu.make_async_copy(txa, txa, ra.at[a]).wait()
            pltpu.make_async_copy(txa, txa, ra.at[b]).wait()
        ta, tb = rxa[tile(a), :], rxa[tile(b), :]
        qs = jnp.where(upper, ta, tb)
        t2 = pltpu.roll(jnp.where(upper, tb, ta), 4, 0)
        even2 = (row & 3) < 2
        fresh_k = jnp.where(even2, t2, pltpu.roll(t2, 2, 0))
        fresh_v = jnp.where(even2, pltpu.roll(t2, 6, 0), t2)
        fresh_score = jnp.sum(qs * fresh_k, axis=1, keepdims=True)
        lhs = jnp.concatenate(
            [jnp.where(upper, ta, 0.0).astype(jnp.bfloat16), jnp.where(upper, 0.0, tb).astype(jnp.bfloat16)], axis=1
        )
        la, lb = len_s[a] - offset, len_s[b] - offset
        limit = jnp.where(upper, la, lb)[:, :1]
        kin[i].wait()
        scores = []
        for c in range(ROWS // 256):
            chunk = pl.ds(c * 256, 256)
            rhs = jnp.concatenate([kbuf[a, chunk, :], kbuf[b, chunk, :]], axis=1)
            s = lax.dot_general(lhs, rhs, (((1,), (1,)), ((), ())), preferred_element_type=jnp.float32)
            place = jnp.where(apart, 1 << 20, c * 128 + (column >> 1))
            s = jnp.where(place == limit, fresh_score, s)
            scores.append((jnp.where(place <= limit, s, FLOOR), place))
        top = scores[0][0]
        for s, _ in scores[1:]:
            top = jnp.maximum(top, s)
        top = jnp.max(top, axis=1, keepdims=True)
        base = jnp.maximum(top, 0.1 * FLOOR)
        total = jnp.zeros((8, 256), jnp.float32)
        weights = []
        for s, place in scores:
            w = jnp.exp(s - base).astype(jnp.bfloat16)
            total = total + w.astype(jnp.float32)
            weights.append(jnp.where(place == limit, 0.0, w.astype(jnp.float32)).astype(jnp.bfloat16))
        total = jnp.sum(total, axis=1, keepdims=True)
        fresh_weight = jnp.exp(fresh_score - base).astype(jnp.bfloat16).astype(jnp.float32)
        fresh_weight = jnp.where((limit >= 0) & (limit < POS), fresh_weight, 0.0)
        vin[i].wait()
        both = jnp.dot(
            jnp.concatenate(weights, axis=1),
            jnp.concatenate([vbuf[a], vbuf[b]], axis=1),
            preferred_element_type=jnp.float32,
        )
        valued = jnp.where(upper, both[:, :128], both[:, 128:])
        obuf[tile(i), :] = valued + fresh_weight * fresh_v
        ml = jnp.where(lane == q, top, jnp.where(lane == q + 64, total, ml))
        if i == PAIRS - 1:
            obuf[tile(PAIRS), :] = ml
        for g, (start, end) in enumerate(GROUPS):
            if min(end, PAIRS) == i + 1:
                for p in kv_peers():
                    pltpu.make_async_remote_copy(
                        obuf.at[tile(start, end - start)],
                        rx2.at[me, tile(start, end - start)],
                        s2.at[g],
                        r2.at[g],
                        device_id=(p, tp),
                        device_id_type=MESH,
                    ).start()
    rx2[me] = obuf[...]

    for c in ins[7:10]:
        c.wait()
    for g, (start, end) in enumerate(GROUPS):
        got = rx2.at[pl.ds(0, N_KV - 1), tile(start, end - start)]
        pltpu.make_async_copy(got, got, r2.at[g]).wait()
    stats = [rx2[s, tile(PAIRS), :] for s in range(N_KV)]
    tops = stats
    while len(tops) > 1:
        tops = [jnp.maximum(a, b) for a, b in zip(tops[::2], tops[1::2])]
    factors = [jnp.exp(s - tops[0]) for s in stats]
    totals = [f * pltpu.roll(s, 64, 1) for f, s in zip(factors, stats)]
    while len(totals) > 1:
        totals = [a + b for a, b in zip(totals[::2], totals[1::2])]
    shares = 1.0 / totals[0]
    second = jnp.where((row & 1) == 1, lam_s[1], lam_s[0])
    for q in range(PAIRS):
        terms = [
            rx2[s, tile(TURN[s][q]), :] * jnp.broadcast_to(factors[s][:, q : q + 1], (8, 128)) for s in range(N_KV)
        ]
        while len(terms) > 1:
            terms = [a + b for a, b in zip(terms[::2], terms[1::2])]
        x = terms[0] * jnp.broadcast_to(shares[:, q : q + 1], (8, 128))
        mixed = x - second * pltpu.roll(x, 6, 0)
        mean = jnp.sum(mixed * mixed, axis=1, keepdims=True) / (2 * DH)
        ho[tile(q), :] = mixed * lax.rsqrt(mean + EPS) * hg_v[...]
    heads = jnp.concatenate(
        [ho[pl.ds(h, SEQS, stride=4), :].astype(jnp.bfloat16) for h in range(2)], axis=1
    )
    part[...] = jnp.dot(heads, wo_v[...], preferred_element_type=jnp.float32)
    for p in tp_peers():
        pltpu.make_async_remote_copy(
            part, rx3.at[tp], s3, r3, device_id=(me, p), device_id_type=MESH
        ).start()
    rx3[tp] = part[...]

    pltpu.make_async_copy(whole, whole, s1).wait()
    pltpu.make_async_copy(whole, whole, sa).wait()
    for i in range(N_KV - 1):
        st = kv_peer(STEPS[i])
    for g, (start, end) in enumerate(GROUPS):
        got = rx2.at[pl.ds(0, N_KV - 1), tile(start, end - start)]
        pltpu.make_async_copy(got, got, s2.at[g]).wait()
    seven = rx3.at[pl.ds(0, N_TP - 1)]
    pltpu.make_async_copy(seven, seven, s3).wait()
    pltpu.make_async_copy(seven, seven, r3).wait()
    sums = [rx3[i] for i in range(N_TP)]
    while len(sums) > 1:
        sums = [a + b for a, b in zip(sums[::2], sums[1::2])]
    out[...] = sums[0].astype(out.dtype)


def local(
    tokens, norm_gain, query_weight, key_weight, value_weight, out_weight, lambdas, head_gain, lengths,
    key_cache, value_cache,
):
    any_space = pl.BlockSpec(memory_space=pl.ANY)
    vmem, dma = pltpu.VMEM, pltpu.SemaphoreType.DMA
    f32, bf16 = jnp.float32, jnp.bfloat16
    return pl.pallas_call(
        kernel,
        out_shape=jax.ShapeDtypeStruct((SEQS, 256), bf16),
        in_specs=[any_space] * 12,
        out_specs=pl.BlockSpec(memory_space=pltpu.VMEM),
        scratch_shapes=[
            vmem((SEQS, 256), bf16), vmem((1, 256), f32), vmem((256, 256), bf16), vmem((256, 256), bf16),
            vmem((256, 256), bf16), vmem((256, 256), bf16), pltpu.SMEM((2,), f32), vmem((1, 128), f32),
            pltpu.SMEM((SEQS,), jnp.int32), vmem((1, 128), f32), vmem((SEQS, ROWS, 128), bf16),
            vmem((SEQS, ROWS, 128), bf16),
            vmem((8 * N_KV, 128), f32), vmem((8 * N_KV, 128), f32), vmem((8, 128), f32), vmem((8 * N_KV, 128), f32),
            vmem((8 * TILES, 128), f32), vmem((N_KV, 8 * TILES, 128), f32), vmem((8 * PAIRS, 128), f32),
            vmem((SEQS, 256), f32), vmem((N_TP, SEQS, 256), f32),
            dma((10,)), dma((PAIRS,)), dma((PAIRS,)), dma, dma, dma, dma((N_KV,)),
            dma((len(GROUPS),)), dma((len(GROUPS),)), dma, dma,
        ],
        compiler_params=pltpu.CompilerParams(
            collective_id=0, has_side_effects=True, vmem_limit_bytes=60000 * 1024
        ),
    )(
        tokens, norm_gain.reshape(1, -1), query_weight, key_weight, value_weight, out_weight, lambdas,
        head_gain.reshape(1, -1), lengths, jnp.asarray(frequencies()),
        key_cache.reshape(SEQS, ROWS, 128), value_cache.reshape(SEQS, ROWS, 128),
    )


def solution(mesh):
    return jax.shard_map(
        local,
        mesh=mesh,
        in_specs=(
            P(None, "kv"),
            P("kv"),
            P("kv", "tp"),
            P("kv", "tp"),
            P("kv", "tp"),
            P("tp", "kv"),
            P("tp"),
            P(),
            P(),
            P(None, "kv", "tp", None),
            P(None, "kv", "tp", None),
        ),
        out_specs=P(None, "kv"),
        check_vma=False,
    )
```

```python
import functools

import jax
import jax.numpy as jnp
import numpy as np
from jax import lax
from jax.experimental import pallas as pl
from jax.experimental.pallas import tpu as pltpu
from jax.sharding import PartitionSpec as P

D = 4096
DH = 64
SEQS = 16
N_KV = 16
N_TP = 8
SIDE = 4
POS = 1024
ROWS = 2 * POS
EPS = 1e-05
THETA = 500000.0
FLOOR = -1e30
MESH = pl.DeviceIdType.MESH

ORDER = ((0, 0), (0, 1), (1, 0), (3, 0), (1, 1), (3, 1), (2, 0), (2, 1))
PAIRS = len(ORDER)
GROUPS = ((0, 3), (3, 5), (5, 7), (7, 9))
TILES = PAIRS + 1
STEPS = sorted(
    ((a, b) for a in range(SIDE) for b in range(SIDE) if a or b),
    key=lambda ab: min(ab[0], SIDE - ab[0]) + min(ab[1], SIDE - ab[1]),
    reverse=True,
)


def frequencies():
    half = DH // 2
    one = np.float64(THETA) ** (-np.arange(half, dtype=np.float64) / half)
    return np.tile(one.astype(np.float32), 2 * 128 // DH)[None, :]


def pair_of(kv, step):
    z, y = kv // SIDE, kv % SIDE
    return ((z + step[0]) % SIDE) * 2 + (y // 2 + step[1]) % 2


TURN = [[[pair_of(kv, st) for st in ORDER].index(q) for q in range(PAIRS)] for kv in range(N_KV)]


def tile(i, n=1):
    start = i * 8
    return pl.ds(start if isinstance(i, int) else pl.multiple_of(start, 8), 8 * n)


def kernel(
    tokens, gain, wq, wk, wv, wo, lambdas, head_gain, lengths, freq, keys, vals,
    out,
    tok_v, gain_v, wq_v, wk_v, wv_v, wo_v, lam_s, hg_v, len_s, freq_v, kbuf, vbuf,
    tx1, rx1, txa, rxa, obuf, rx2, ho, part, rx3,
    in_sem, k_sem, v_sem, s1, r1, sa, ra, s2, r2, s3, r3,
):
    me = lax.axis_index("kv")
    tp = lax.axis_index("tp")
    z, y = me // SIDE, me % SIDE

    def kv_peer(step):
        return ((z + step[0]) % SIDE) * SIDE + (y + step[1]) % SIDE

    def kv_peers():
        return [kv_peer(st) for st in STEPS]

    def tp_peers():
        return [(tp + d) % N_TP for d in range(1, N_TP)]

    barrier = pltpu.get_barrier_semaphore()
    for p in kv_peers():
        pl.semaphore_signal(barrier, 1, device_id=(p, tp), device_id_type=MESH)
    for p in tp_peers():
        pl.semaphore_signal(barrier, 1, device_id=(me, p), device_id_type=MESH)

    ins = [
        pltpu.make_async_copy(src, dst, in_sem.at[i])
        for i, (src, dst) in enumerate(
            (
                (tokens, tok_v), (gain, gain_v), (wq, wq_v), (wk, wk_v), (wv, wv_v), (lengths, len_s),
                (freq, freq_v), (lambdas, lam_s), (head_gain, hg_v), (wo, wo_v),
            )
        )
    ]
    for c in ins:
        c.start()
    pair_at = [pair_of(me, st) for st in ORDER]
    kin, vin = [], []
    for i, q in enumerate(pair_at):
        rows = pl.ds(2 * q, 2)
        kin.append(pltpu.make_async_copy(keys.at[rows], kbuf.at[rows], k_sem.at[i]))
        vin.append(pltpu.make_async_copy(vals.at[rows], vbuf.at[rows], v_sem.at[i]))
    for a, b in zip(kin, vin):
        a.start()
        b.start()

    lane = lax.broadcasted_iota(jnp.int32, (8, 128), 1)
    row = lax.broadcasted_iota(jnp.int32, (8, 128), 0)

    for c in ins[:2]:
        c.wait()
    widened = tok_v[...].astype(jnp.float32)
    squares = jnp.sum(widened * widened, axis=1, keepdims=True)
    normed = (widened * gain_v[...]).astype(jnp.bfloat16)
    low = lax.broadcasted_iota(jnp.int32, (SEQS, 128), 1) < DH
    ins[2].wait()
    q_part = jnp.dot(normed, wq_v[...], preferred_element_type=jnp.float32)
    ins[3].wait()
    k_part = jnp.dot(normed, wk_v[...], preferred_element_type=jnp.float32)
    ins[4].wait()
    v_part = jnp.dot(normed, wv_v[...], preferred_element_type=jnp.float32)
    q0, q1 = q_part[:, :128], q_part[:, 128:]
    lines = (
        jnp.where(low, q0, squares), jnp.where(low, q1, 0.0), jnp.where(low, 0.0, q0), jnp.where(low, 0.0, q1),
        k_part[:, :128], k_part[:, 128:], v_part[:, :128], v_part[:, 128:],
    )
    for i, line in enumerate(lines):
        tx1[pl.ds(i, SEQS, stride=8), :] = line

    pl.semaphore_wait(barrier, N_KV - 1 + N_TP - 1)

    for p in kv_peers():
        pltpu.make_async_remote_copy(
            tx1.at[tile(p)], rx1.at[tile(me)], s1, r1, device_id=(p, tp), device_id_type=MESH
        ).start()
    rx1[tile(me), :] = tx1[tile(me), :]

    ins[5].wait()
    ins[6].wait()
    own_length = len_s[me]
    angles = own_length.astype(jnp.float32) * freq_v[...]
    first = (lane & 32) == 0
    turned = row < 6
    cosine = jnp.where(turned, jnp.broadcast_to(jnp.cos(angles), (8, 128)), 1.0)
    sine = jnp.broadcast_to(jnp.sin(angles), (8, 128))
    sine = jnp.where(turned, jnp.where(first, -sine, sine), 0.0)

    whole = tx1.at[tile(0, N_KV - 1)]
    pltpu.make_async_copy(whole, whole, r1).wait()
    sums = [rx1[tile(i), :] for i in range(N_KV)]
    while len(sums) > 1:
        sums = [a + b for a, b in zip(sums[::2], sums[1::2])]
    summed = sums[0]
    scaling = lax.rsqrt(summed[0:1, DH : DH + 1] / D + EPS)
    x = jnp.where((row == 0) & (lane >= DH), 0.0, summed) * scaling
    other = jnp.where(first, pltpu.roll(x, 96, 1), pltpu.roll(x, 32, 1))
    x = (x * cosine + other * sine).astype(jnp.bfloat16).astype(jnp.float32)
    x = jnp.where(row < 4, x * DH ** (-0.5), x)
    x = jnp.where(lax.broadcast(me % 2, (8, 128)) == 1, pltpu.roll(x, 4, 0), x)
    txa[...] = x
    for p in kv_peers():
        pltpu.make_async_remote_copy(
            txa, rxa.at[tile(me)], sa, ra.at[me], device_id=(p, tp), device_id_type=MESH
        ).start()
    rxa[tile(me), :] = x

    for c in kin + vin:
        c.wait()

    column = lax.broadcasted_iota(jnp.int32, (8, 256), 1)
    crow = lax.broadcasted_iota(jnp.int32, (8, 256), 0)
    apart = ((column ^ crow) & 1) == 1
    offset = me * POS
    upper = row < 4

    def scored(i):
        q = pair_at[i]
        a, b = 2 * q, 2 * q + 1
        ta, tb = rxa[tile(a), :], rxa[tile(b), :]
        qs = jnp.where(upper, ta, tb)
        t2 = pltpu.roll(jnp.where(upper, tb, ta), 4, 0)
        even2 = (row & 3) < 2
        fresh_k = jnp.where(even2, t2, pltpu.roll(t2, 2, 0))
        fresh_v = jnp.where(even2, pltpu.roll(t2, 6, 0), t2)
        fresh_score = jnp.sum(qs * fresh_k, axis=1, keepdims=True)
        lhs = jnp.concatenate(
            [jnp.where(upper, ta, 0.0).astype(jnp.bfloat16), jnp.where(upper, 0.0, tb).astype(jnp.bfloat16)], axis=1
        )
        la, lb = len_s[a] - offset, len_s[b] - offset
        limit = jnp.where(upper, la, lb)[:, :1]
        scores = []
        for c in range(ROWS // 256):
            chunk = pl.ds(c * 256, 256)
            rhs = jnp.concatenate([kbuf[a, chunk, :], kbuf[b, chunk, :]], axis=1)
            scores.append(
                lax.dot_general(lhs, rhs, (((1,), (1,)), ((), ())), preferred_element_type=jnp.float32)
            )
        return scores, fresh_score, fresh_v, limit

    def weighed(i, given, ml):
        q = pair_at[i]
        scores, fresh_score, fresh_v, limit = given
        places = [jnp.where(apart, 1 << 20, c * 128 + (column >> 1)) for c in range(len(scores))]
        scores = [jnp.where(p == limit, fresh_score, s) for p, s in zip(places, scores)]
        scores = [jnp.where(p <= limit, s, FLOOR) for p, s in zip(places, scores)]
        tops = scores
        while len(tops) > 1:
            tops = [jnp.maximum(x, y) for x, y in zip(tops[::2], tops[1::2])]
        top = jnp.max(tops[0], axis=1, keepdims=True)
        base = jnp.maximum(top, 0.1 * FLOOR)
        weights = [jnp.exp(s - base).astype(jnp.bfloat16).astype(jnp.float32) for s in scores]
        cached = [jnp.where(p == limit, 0.0, w).astype(jnp.bfloat16) for p, w in zip(places, weights)]
        totals = weights
        while len(totals) > 1:
            totals = [x + y for x, y in zip(totals[::2], totals[1::2])]
        total = jnp.sum(totals[0], axis=1, keepdims=True)
        fresh_weight = jnp.exp(fresh_score - base).astype(jnp.bfloat16).astype(jnp.float32)
        fresh_weight = jnp.where((limit >= 0) & (limit < POS), fresh_weight, 0.0)
        both = jnp.dot(
            jnp.concatenate(cached, axis=1),
            jnp.concatenate([vbuf[2 * q], vbuf[2 * q + 1]], axis=1),
            preferred_element_type=jnp.float32,
        )
        valued = jnp.where(upper, both[:, :128], both[:, 128:])
        obuf[tile(i), :] = valued + fresh_weight * fresh_v
        return jnp.where(lane == q, top, jnp.where(lane == q + 64, total, ml))

    def sent(i):
        for g, (start, end) in enumerate(GROUPS):
            if min(end, PAIRS) == i + 1:
                for p in kv_peers():
                    pltpu.make_async_remote_copy(
                        obuf.at[tile(start, end - start)],
                        rx2.at[me, tile(start, end - start)],
                        s2.at[g],
                        r2.at[g],
                        device_id=(p, tp),
                        device_id_type=MESH,
                    ).start()

    ml = jnp.zeros((8, 128), jnp.float32)
    ahead = None
    for i, q in enumerate(pair_at):
        if i == 0:
            pltpu.make_async_copy(txa, txa, ra.at[me + 1 - 2 * (me % 2)]).wait()
        else:
            pltpu.make_async_copy(txa, txa, ra.at[2 * q]).wait()
            pltpu.make_async_copy(txa, txa, ra.at[2 * q + 1]).wait()
        now = scored(i)
        if i:
            ml = weighed(i - 1, ahead, ml)
            sent(i - 1)
        ahead = now
    ml = weighed(PAIRS - 1, ahead, ml)
    obuf[tile(PAIRS), :] = ml
    sent(PAIRS - 1)
    rx2[me] = obuf[...]

    for c in ins[7:10]:
        c.wait()
    for g, (start, end) in enumerate(GROUPS):
        got = rx2.at[pl.ds(0, N_KV - 1), tile(start, end - start)]
        pltpu.make_async_copy(got, got, r2.at[g]).wait()
    stats = [rx2[s, tile(PAIRS), :] for s in range(N_KV)]
    tops = stats
    while len(tops) > 1:
        tops = [jnp.maximum(a, b) for a, b in zip(tops[::2], tops[1::2])]
    factors = [jnp.exp(s - tops[0]) for s in stats]
    totals = [f * pltpu.roll(s, 64, 1) for f, s in zip(factors, stats)]
    while len(totals) > 1:
        totals = [a + b for a, b in zip(totals[::2], totals[1::2])]
    shares = 1.0 / totals[0]
    second = jnp.where((row & 1) == 1, lam_s[1], lam_s[0])
    for q in range(PAIRS):
        terms = [
            rx2[s, tile(TURN[s][q]), :] * jnp.broadcast_to(factors[s][:, q : q + 1], (8, 128)) for s in range(N_KV)
        ]
        while len(terms) > 1:
            terms = [a + b for a, b in zip(terms[::2], terms[1::2])]
        x = terms[0] * jnp.broadcast_to(shares[:, q : q + 1], (8, 128))
        mixed = x - second * pltpu.roll(x, 6, 0)
        mean = jnp.sum(mixed * mixed, axis=1, keepdims=True) / (2 * DH)
        ho[tile(q), :] = mixed * lax.rsqrt(mean + EPS) * hg_v[...]
    heads = jnp.concatenate(
        [ho[pl.ds(h, SEQS, stride=4), :].astype(jnp.bfloat16) for h in range(2)], axis=1
    )
    part[...] = jnp.dot(heads, wo_v[...], preferred_element_type=jnp.float32)
    for p in tp_peers():
        pltpu.make_async_remote_copy(
            part, rx3.at[tp], s3, r3, device_id=(me, p), device_id_type=MESH
        ).start()
    rx3[tp] = part[...]

    pltpu.make_async_copy(whole, whole, s1).wait()
    pltpu.make_async_copy(whole, whole, sa).wait()
    for g, (start, end) in enumerate(GROUPS):
        got = rx2.at[pl.ds(0, N_KV - 1), tile(start, end - start)]
        pltpu.make_async_copy(got, got, s2.at[g]).wait()
    seven = rx3.at[pl.ds(0, N_TP - 1)]
    pltpu.make_async_copy(seven, seven, s3).wait()
    pltpu.make_async_copy(seven, seven, r3).wait()
    sums = [rx3[i] for i in range(N_TP)]
    while len(sums) > 1:
        sums = [a + b for a, b in zip(sums[::2], sums[1::2])]
    out[...] = sums[0].astype(out.dtype)


def local(
    tokens, norm_gain, query_weight, key_weight, value_weight, out_weight, lambdas, head_gain, lengths,
    key_cache, value_cache,
):
    any_space = pl.BlockSpec(memory_space=pl.ANY)
    vmem, dma = pltpu.VMEM, pltpu.SemaphoreType.DMA
    f32, bf16 = jnp.float32, jnp.bfloat16
    return pl.pallas_call(
        kernel,
        out_shape=pltpu.VMEM((SEQS, 256), bf16),
        in_specs=[any_space] * 12,
        out_specs=pl.BlockSpec(memory_space=pltpu.VMEM),
        scratch_shapes=[
            vmem((SEQS, 256), bf16), vmem((1, 256), f32), vmem((256, 256), bf16), vmem((256, 256), bf16),
            vmem((256, 256), bf16), vmem((256, 256), bf16), pltpu.SMEM((2,), f32), vmem((1, 128), f32),
            pltpu.SMEM((SEQS,), jnp.int32), vmem((1, 128), f32), vmem((SEQS, ROWS, 128), bf16),
            vmem((SEQS, ROWS, 128), bf16),
            vmem((8 * N_KV, 128), f32), vmem((8 * N_KV, 128), f32), vmem((8, 128), f32), vmem((8 * N_KV, 128), f32),
            vmem((8 * TILES, 128), f32), vmem((N_KV, 8 * TILES, 128), f32), vmem((8 * PAIRS, 128), f32),
            vmem((SEQS, 256), f32), vmem((N_TP, SEQS, 256), f32),
            dma((10,)), dma((PAIRS,)), dma((PAIRS,)), dma, dma, dma, dma((N_KV,)),
            dma((len(GROUPS),)), dma((len(GROUPS),)), dma, dma,
        ],
        compiler_params=pltpu.CompilerParams(
            collective_id=0, has_side_effects=True, vmem_limit_bytes=60000 * 1024
        ),
    )(
        tokens, norm_gain.reshape(1, -1), query_weight, key_weight, value_weight, out_weight, lambdas,
        head_gain.reshape(1, -1), lengths, jnp.asarray(frequencies()),
        key_cache.reshape(SEQS, ROWS, 128), value_cache.reshape(SEQS, ROWS, 128),
    )


def solution(mesh):
    return jax.shard_map(
        local,
        mesh=mesh,
        in_specs=(
            P(None, "kv"),
            P("kv"),
            P("kv", "tp"),
            P("kv", "tp"),
            P("kv", "tp"),
            P("tp", "kv"),
            P("tp"),
            P(),
            P(),
            P(None, "kv", "tp", None),
            P(None, "kv", "tp", None),
        ),
        out_specs=P(None, "kv"),
        check_vma=False,
    )
```

```python
import functools

import jax
import jax.numpy as jnp
import numpy as np
from jax import lax
from jax.experimental import pallas as pl
from jax.experimental.pallas import tpu as pltpu
from jax.sharding import PartitionSpec as P

D = 4096
DH = 64
SEQS = 16
N_KV = 16
N_TP = 8
SIDE = 4
POS = 1024
ROWS = 2 * POS
CHUNKS = ROWS // 256
EPS = 1e-05
THETA = 500000.0
FLOOR = -1e30
MESH = pl.DeviceIdType.MESH

ORDER = ((0, 0), (0, 1), (1, 0), (3, 0), (1, 1), (3, 1), (2, 0), (2, 1))
PAIRS = len(ORDER)
GROUPS = ((0, 3), (3, 5), (5, 7), (7, 9))
TILES = PAIRS + 1
STEPS = sorted(
    ((a, b) for a in range(SIDE) for b in range(SIDE) if a or b),
    key=lambda ab: min(ab[0], SIDE - ab[0]) + min(ab[1], SIDE - ab[1]),
    reverse=True,
)


def frequencies():
    half = DH // 2
    one = np.float64(THETA) ** (-np.arange(half, dtype=np.float64) / half)
    return np.tile(one.astype(np.float32), 2 * 128 // DH)[None, :]


def pair_of(kv, step):
    z, y = kv // SIDE, kv % SIDE
    return ((z + step[0]) % SIDE) * 2 + (y // 2 + step[1]) % 2


TURN = [[[pair_of(kv, st) for st in ORDER].index(q) for q in range(PAIRS)] for kv in range(N_KV)]


def tile(i, n=1):
    start = i * 8
    return pl.ds(start if isinstance(i, int) else pl.multiple_of(start, 8), 8 * n)


def kernel(
    tokens, gain, wq, wk, wv, wo, lambdas, head_gain, lengths, freq, keys, vals,
    out,
    tok_v, gain_v, wq_v, wk_v, wv_v, wo_v, lam_s, hg_v, len_s, freq_v, kbuf, vbuf,
    tx1, rx1, txa, rxa, obuf, rx2, ho, part, rx3,
    in_sem, k_sem, v_sem, s1, r1, sa, ra, s2, r2, s3, r3,
    *, score_sums, value_sums,
):
    me = lax.axis_index("kv")
    tp = lax.axis_index("tp")
    z, y = me // SIDE, me % SIDE

    def kv_peer(step):
        return ((z + step[0]) % SIDE) * SIDE + (y + step[1]) % SIDE

    def kv_peers():
        return [kv_peer(st) for st in STEPS]

    def tp_peers():
        return [(tp + d) % N_TP for d in range(1, N_TP)]

    barrier = pltpu.get_barrier_semaphore()
    for p in kv_peers():
        pl.semaphore_signal(barrier, 1, device_id=(p, tp), device_id_type=MESH)
    for p in tp_peers():
        pl.semaphore_signal(barrier, 1, device_id=(me, p), device_id_type=MESH)

    ins = [
        pltpu.make_async_copy(src, dst, in_sem.at[i])
        for i, (src, dst) in enumerate(
            (
                (tokens, tok_v), (gain, gain_v), (wq, wq_v), (wk, wk_v), (wv, wv_v), (lengths, len_s),
                (freq, freq_v), (lambdas, lam_s), (head_gain, hg_v), (wo, wo_v),
            )
        )
    ]
    for c in ins:
        c.start()
    pair_at = [pair_of(me, st) for st in ORDER]
    kin, vin = [], []
    for i, q in enumerate(pair_at):
        rows = pl.ds(2 * q, 2)
        kin.append(pltpu.make_async_copy(keys.at[rows], kbuf.at[rows], k_sem.at[i]))
        vin.append(pltpu.make_async_copy(vals.at[rows], vbuf.at[rows], v_sem.at[i]))
    for a, b in zip(kin, vin):
        a.start()
        b.start()

    register = [0, 0]

    def multiply(unit, sums, left, right, transpose=False):
        pltpu.matmul_push_rhs(right, staging_register=register[unit], mxu_index=unit, transpose=transpose)
        pltpu.matmul_acc_lhs(sums, left, load_staged_rhs=register[unit])
        register[unit] ^= 1

    for unit in range(2):
        for sums in (*score_sums[unit][0], *score_sums[unit][1], *value_sums[unit]):
            pltpu.matmul_pop(sums)

    lane = lax.broadcasted_iota(jnp.int32, (8, 128), 1)
    row = lax.broadcasted_iota(jnp.int32, (8, 128), 0)

    for c in ins[:2]:
        c.wait()
    widened = tok_v[...].astype(jnp.float32)
    squares = jnp.sum(widened * widened, axis=1, keepdims=True)
    normed = (widened * gain_v[...]).astype(jnp.bfloat16)
    low = lax.broadcasted_iota(jnp.int32, (SEQS, 128), 1) < DH
    weights = (wq_v, wk_v, wv_v)
    for i, w in enumerate(weights):
        ins[2 + i].wait()
        multiply(i % 2, score_sums[i % 2][0][i], normed, w[...])
    q_part, k_part, v_part = [pltpu.matmul_pop(score_sums[i % 2][0][i]) for i in range(3)]
    q0, q1 = q_part[:, :128], q_part[:, 128:]
    lines = (
        jnp.where(low, q0, squares), jnp.where(low, q1, 0.0), jnp.where(low, 0.0, q0), jnp.where(low, 0.0, q1),
        k_part[:, :128], k_part[:, 128:], v_part[:, :128], v_part[:, 128:],
    )
    for i, line in enumerate(lines):
        tx1[pl.ds(i, SEQS, stride=8), :] = line

    pl.semaphore_wait(barrier, N_KV - 1 + N_TP - 1)

    for p in kv_peers():
        pltpu.make_async_remote_copy(
            tx1.at[tile(p)], rx1.at[tile(me)], s1, r1, device_id=(p, tp), device_id_type=MESH
        ).start()
    rx1[tile(me), :] = tx1[tile(me), :]

    ins[5].wait()
    ins[6].wait()
    own_length = len_s[me]
    angles = own_length.astype(jnp.float32) * freq_v[...]
    first = (lane & 32) == 0
    turned = row < 6
    cosine = jnp.where(turned, jnp.broadcast_to(jnp.cos(angles), (8, 128)), 1.0)
    sine = jnp.broadcast_to(jnp.sin(angles), (8, 128))
    sine = jnp.where(turned, jnp.where(first, -sine, sine), 0.0)

    whole = tx1.at[tile(0, N_KV - 1)]
    pltpu.make_async_copy(whole, whole, r1).wait()
    sums = [rx1[tile(i), :] for i in range(N_KV)]
    while len(sums) > 1:
        sums = [a + b for a, b in zip(sums[::2], sums[1::2])]
    summed = sums[0]
    scaling = lax.rsqrt(summed[0:1, DH : DH + 1] / D + EPS)
    x = jnp.where((row == 0) & (lane >= DH), 0.0, summed) * scaling
    other = jnp.where(first, pltpu.roll(x, 96, 1), pltpu.roll(x, 32, 1))
    x = (x * cosine + other * sine).astype(jnp.bfloat16).astype(jnp.float32)
    x = jnp.where(row < 4, x * DH ** (-0.5), x)
    x = jnp.where(lax.broadcast(me % 2, (8, 128)) == 1, pltpu.roll(x, 4, 0), x)
    txa[...] = x
    for p in kv_peers():
        pltpu.make_async_remote_copy(
            txa, rxa.at[tile(me)], sa, ra.at[me], device_id=(p, tp), device_id_type=MESH
        ).start()
    rxa[tile(me), :] = x

    for c in kin + vin:
        c.wait()

    column = lax.broadcasted_iota(jnp.int32, (8, 256), 1)
    crow = lax.broadcasted_iota(jnp.int32, (8, 256), 0)
    apart = ((column ^ crow) & 1) == 1
    offset = me * POS
    upper = row < 4

    blank = jnp.zeros((8, 256), jnp.float32)

    def left_side(x):
        return jnp.concatenate([x, blank], axis=0).astype(jnp.bfloat16)

    def prepared(i):
        q = pair_at[i]
        a, b = 2 * q, 2 * q + 1
        ta, tb = rxa[tile(a), :], rxa[tile(b), :]
        left = left_side(jnp.concatenate([jnp.where(upper, ta, 0.0), jnp.where(upper, 0.0, tb)], axis=1))
        for c in range(CHUNKS):
            chunk = pl.ds(c * 256, 256)
            right = jnp.concatenate([kbuf[a, chunk, :], kbuf[b, chunk, :]], axis=1)
            multiply(c % 2, score_sums[c % 2][i % 2][c // 2], left, right, True)
        qs = jnp.where(upper, ta, tb)
        t2 = pltpu.roll(jnp.where(upper, tb, ta), 4, 0)
        even2 = (row & 3) < 2
        fresh_k = jnp.where(even2, t2, pltpu.roll(t2, 2, 0))
        fresh_v = jnp.where(even2, pltpu.roll(t2, 6, 0), t2)
        fresh_score = jnp.sum(qs * fresh_k, axis=1, keepdims=True)
        la, lb = len_s[a] - offset, len_s[b] - offset
        return fresh_score, fresh_v, jnp.where(upper, la, lb)[:, :1]

    def weighed(i, given):
        q = pair_at[i]
        fresh_score, fresh_v, limit = given
        scores = [pltpu.matmul_pop(score_sums[c % 2][i % 2][c // 2])[:8] for c in range(CHUNKS)]
        places = [jnp.where(apart, 1 << 20, c * 128 + (column >> 1)) for c in range(CHUNKS)]
        scores = [jnp.where(p == limit, fresh_score, s) for p, s in zip(places, scores)]
        scores = [jnp.where(p <= limit, s, FLOOR) for p, s in zip(places, scores)]
        tops = scores
        while len(tops) > 1:
            tops = [jnp.maximum(x, y) for x, y in zip(tops[::2], tops[1::2])]
        top = jnp.max(tops[0], axis=1, keepdims=True)
        base = jnp.maximum(top, 0.1 * FLOOR)
        weights = [jnp.exp(s - base).astype(jnp.bfloat16).astype(jnp.float32) for s in scores]
        for c in range(CHUNKS):
            chunk = pl.ds(c * 256, 256)
            right = jnp.concatenate([vbuf[2 * q, chunk, :], vbuf[2 * q + 1, chunk, :]], axis=1)
            cached = jnp.where(places[c] == limit, 0.0, weights[c])
            multiply(c % 2, value_sums[c % 2][i % 2], left_side(cached), right)
        totals = weights
        while len(totals) > 1:
            totals = [x + y for x, y in zip(totals[::2], totals[1::2])]
        total = jnp.sum(totals[0], axis=1, keepdims=True)
        fresh_weight = jnp.exp(fresh_score - base).astype(jnp.bfloat16).astype(jnp.float32)
        fresh_weight = jnp.where((limit >= 0) & (limit < POS), fresh_weight, 0.0)
        return top, total, fresh_weight * fresh_v

    def finished(i, given, ml):
        q = pair_at[i]
        top, total, fresh = given
        both = pltpu.matmul_pop(value_sums[0][i % 2])[:8] + pltpu.matmul_pop(value_sums[1][i % 2])[:8]
        obuf[tile(i), :] = jnp.where(upper, both[:, :128], both[:, 128:]) + fresh
        ml = jnp.where(lane == q, top, jnp.where(lane == q + 64, total, ml))
        if i == PAIRS - 1:
            obuf[tile(PAIRS), :] = ml
        sent(i)
        return ml

    def sent(i):
        for g, (start, end) in enumerate(GROUPS):
            if min(end, PAIRS) == i + 1:
                for p in kv_peers():
                    pltpu.make_async_remote_copy(
                        obuf.at[tile(start, end - start)],
                        rx2.at[me, tile(start, end - start)],
                        s2.at[g],
                        r2.at[g],
                        device_id=(p, tp),
                        device_id_type=MESH,
                    ).start()

    ml = jnp.zeros((8, 128), jnp.float32)
    scored, valued = None, None
    for i in range(PAIRS + 2):
        now = None
        if i == 0:
            pltpu.make_async_copy(txa, txa, ra.at[me + 1 - 2 * (me % 2)]).wait()
        elif i < PAIRS:
            pltpu.make_async_copy(txa, txa, ra.at[2 * pair_at[i]]).wait()
            pltpu.make_async_copy(txa, txa, ra.at[2 * pair_at[i] + 1]).wait()
        if i < PAIRS:
            now = prepared(i)
        if i >= 2:
            ml = finished(i - 2, valued, ml)
        valued = weighed(i - 1, scored) if 1 <= i <= PAIRS else None
        scored = now
    rx2[me] = obuf[...]

    for c in ins[7:10]:
        c.wait()
    for g, (start, end) in enumerate(GROUPS):
        got = rx2.at[pl.ds(0, N_KV - 1), tile(start, end - start)]
        pltpu.make_async_copy(got, got, r2.at[g]).wait()
    stats = [rx2[s, tile(PAIRS), :] for s in range(N_KV)]
    tops = stats
    while len(tops) > 1:
        tops = [jnp.maximum(a, b) for a, b in zip(tops[::2], tops[1::2])]
    factors = [jnp.exp(s - tops[0]) for s in stats]
    totals = [f * pltpu.roll(s, 64, 1) for f, s in zip(factors, stats)]
    while len(totals) > 1:
        totals = [a + b for a, b in zip(totals[::2], totals[1::2])]
    shares = 1.0 / totals[0]
    second = jnp.where((row & 1) == 1, lam_s[1], lam_s[0])
    for q in range(PAIRS):
        terms = [
            rx2[s, tile(TURN[s][q]), :] * jnp.broadcast_to(factors[s][:, q : q + 1], (8, 128)) for s in range(N_KV)
        ]
        while len(terms) > 1:
            terms = [a + b for a, b in zip(terms[::2], terms[1::2])]
        x = terms[0] * jnp.broadcast_to(shares[:, q : q + 1], (8, 128))
        mixed = x - second * pltpu.roll(x, 6, 0)
        mean = jnp.sum(mixed * mixed, axis=1, keepdims=True) / (2 * DH)
        ho[tile(q), :] = mixed * lax.rsqrt(mean + EPS) * hg_v[...]
    heads = jnp.concatenate(
        [ho[pl.ds(h, SEQS, stride=4), :].astype(jnp.bfloat16) for h in range(2)], axis=1
    )
    multiply(0, value_sums[0][0], heads, wo_v[...])
    part[...] = pltpu.matmul_pop(value_sums[0][0])
    for p in tp_peers():
        pltpu.make_async_remote_copy(
            part, rx3.at[tp], s3, r3, device_id=(me, p), device_id_type=MESH
        ).start()
    rx3[tp] = part[...]

    pltpu.make_async_copy(whole, whole, s1).wait()
    pltpu.make_async_copy(whole, whole, sa).wait()
    for g, (start, end) in enumerate(GROUPS):
        got = rx2.at[pl.ds(0, N_KV - 1), tile(start, end - start)]
        pltpu.make_async_copy(got, got, s2.at[g]).wait()
    seven = rx3.at[pl.ds(0, N_TP - 1)]
    pltpu.make_async_copy(seven, seven, s3).wait()
    pltpu.make_async_copy(seven, seven, r3).wait()
    sums = [rx3[i] for i in range(N_TP)]
    while len(sums) > 1:
        sums = [a + b for a, b in zip(sums[::2], sums[1::2])]
    out[...] = sums[0].astype(out.dtype)


def with_sums(*refs):
    kinds = [pltpu.ACC(unit)((16, 256), jnp.float32) for unit in range(2) for _ in range(CHUNKS + 2)]

    def body(*sums):
        units = sums[: CHUNKS + 2], sums[CHUNKS + 2 :]
        half = CHUNKS // 2
        kernel(
            *refs,
            score_sums=[(u[:half], u[half:CHUNKS]) for u in units],
            value_sums=[u[CHUNKS:] for u in units],
        )

    pl.run_scoped(body, *kinds)


def local(
    tokens, norm_gain, query_weight, key_weight, value_weight, out_weight, lambdas, head_gain, lengths,
    key_cache, value_cache,
):
    any_space = pl.BlockSpec(memory_space=pl.ANY)
    vmem, dma = pltpu.VMEM, pltpu.SemaphoreType.DMA
    f32, bf16 = jnp.float32, jnp.bfloat16
    return pl.pallas_call(
        with_sums,
        out_shape=pltpu.VMEM((SEQS, 256), bf16),
        in_specs=[any_space] * 12,
        out_specs=pl.BlockSpec(memory_space=pltpu.VMEM),
        scratch_shapes=[
            vmem((SEQS, 256), bf16), vmem((1, 256), f32), vmem((256, 256), bf16), vmem((256, 256), bf16),
            vmem((256, 256), bf16), vmem((256, 256), bf16), pltpu.SMEM((2,), f32), vmem((1, 128), f32),
            pltpu.SMEM((SEQS,), jnp.int32), vmem((1, 128), f32), vmem((SEQS, ROWS, 128), bf16),
            vmem((SEQS, ROWS, 128), bf16),
            vmem((8 * N_KV, 128), f32), vmem((8 * N_KV, 128), f32), vmem((8, 128), f32), vmem((8 * N_KV, 128), f32),
            vmem((8 * TILES, 128), f32), vmem((N_KV, 8 * TILES, 128), f32), vmem((8 * PAIRS, 128), f32),
            vmem((SEQS, 256), f32), vmem((N_TP, SEQS, 256), f32),
            dma((10,)), dma((PAIRS,)), dma((PAIRS,)), dma, dma, dma, dma((N_KV,)),
            dma((len(GROUPS),)), dma((len(GROUPS),)), dma, dma,
        ],
        compiler_params=pltpu.CompilerParams(
            collective_id=0, has_side_effects=True, vmem_limit_bytes=60000 * 1024
        ),
    )(
        tokens, norm_gain.reshape(1, -1), query_weight, key_weight, value_weight, out_weight, lambdas,
        head_gain.reshape(1, -1), lengths, jnp.asarray(frequencies()),
        key_cache.reshape(SEQS, ROWS, 128), value_cache.reshape(SEQS, ROWS, 128),
    )


def solution(mesh):
    return jax.shard_map(
        local,
        mesh=mesh,
        in_specs=(
            P(None, "kv"),
            P("kv"),
            P("kv", "tp"),
            P("kv", "tp"),
            P("kv", "tp"),
            P("tp", "kv"),
            P("tp"),
            P(),
            P(),
            P(None, "kv", "tp", None),
            P(None, "kv", "tp", None),
        ),
        out_specs=P(None, "kv"),
        check_vma=False,
    )
```
